32 devices in a mesh: grp: 2 (over y), dp: 2 (over x), kv: 4 (over z), tp: 2 (over core).
Axes of the slice: x: 2, y: 2, z: 4, core: 2. Of those that a mesh axis runs over, the one named last changes fastest.
Arguments:
- tokens: bfloat16 [32, 2048], P(('grp', 'dp'), ('kv', 'tp')), parts along dimension 0, may hold values from -24 to 24
- memory: float32 [32, 12, 16384], P(('grp', 'dp', 'kv', 'tp')), parts along dimension 0, may hold values from -3 to 3
- mix_gain: float32 [2048], replicated, may hold values from 0.1 to 1.9
- w_query: bfloat16 [2048, 1536], P(None, ('kv', 'tp')), may hold values from -0.125 to 0.125
- w_key: bfloat16 [2048, 1536], P(None, ('kv', 'tp')), may hold values from -0.125 to 0.125
- w_value: bfloat16 [2048, 1536], P(None, ('kv', 'tp')), may hold values from -0.125 to 0.125
- w_gate: bfloat16 [2048, 1536], P(None, ('kv', 'tp')), may hold values from -0.125 to 0.125
- w_beta: bfloat16 [2048, 12], replicated, may hold values from -0.125 to 0.125
- w_decay: bfloat16 [2048, 12], replicated, may hold values from -0.125 to 0.125
- decay_rate: float32 [12], replicated, may hold values from 0.1 to 3
- decay_bias: float32 [12], replicated, may hold values from -2 to 1
- head_gain: float32 [128], replicated, may hold values from 0.1 to 1.9
- w_out: bfloat16 [1536, 2048], P(None, ('kv', 'tp')), may hold values from -0.15625 to 0.15625
- ffn_gain: float32 [2048], replicated, may hold values from 0.1 to 1.9
- w_up: bfloat16 [2048, 8192], P(None, ('kv', 'tp')), may hold values from -0.125 to 0.125
- w_down: bfloat16 [8192, 2048], P(('kv', 'tp')), may hold values from -0.09375 to 0.09375
Outputs:
- layer_out: bfloat16 [32, 2048], P(('grp', 'dp'), ('kv', 'tp')), parts along dimension 0
- new_memory: float32 [32, 12, 16384], P(('grp', 'dp', 'kv', 'tp')), parts along dimension 0
The draws below stay inside these ranges and needn't reach their ends.
There are 2 independent parts, one for each index of `grp`. The reference program is written for one: setup_inputs(seed, part) draws one part's arguments, and reference() takes and returns one part's arrays. A program takes and returns all parts, laid end to end along the dimension named above; an argument that names none is the same for every part. Nothing has to cross between parts.
All inputs are finite; a program needn't handle non-finite values.
Results may differ from the reference program's by a relative error of at most 0.02.
Values may be sent and summed in bfloat16 or wider, within the bound.
A program may use at most 64 MiB of HBM per device.

```python
import math
import jax
import jax.numpy as jnp
from jax import lax

D = 2048
HEADS = 12
HEAD_DIM = 128
FF = 8192
BATCH = 16


def draw_tokens(key, part):
    streams = jax.random.split(key, 3)
    trend = jnp.exp(jnp.linspace(math.log(0.5), math.log(1.5), D)).astype(jnp.float32)
    rough = jnp.exp(jax.random.uniform(streams[0], (D,), jnp.float32, -0.5, 0.5))
    row_scale = jnp.exp(jax.random.uniform(streams[1], (BATCH, 1), jnp.float32, -0.7, 0.7))
    base = jax.random.normal(streams[2], (BATCH, D), jnp.float32)
    values = jnp.clip(base * row_scale * trend * rough, -24.0, 24.0)
    return values.astype(jnp.bfloat16)


def strengthened(drawn, stream_key, source, target, shards_of, factor):
    owner, partner = [(jnp.arange(drawn.shape[axis_at]) // (drawn.shape[axis_at] // shards_of)).reshape([-1 if axis == axis_at else 1 for axis in range(drawn.ndim)]) for axis_at in (source, target)]
    chosen = jax.random.permutation(stream_key, shards_of)[partner]
    strong = (owner == chosen) | (owner == (partner + shards_of // 2) % shards_of)
    return jnp.where(strong, factor * drawn, drawn)


def levels(key, dims, shards, low, largest):
    factor_of = 1.0
    for dim, shards_of in shards:
        steps = jax.random.uniform(jax.random.fold_in(jax.random.fold_in(key, 6), dim), (shards_of,), jnp.float32, low / len(shards), largest / len(shards))
        factor_of = factor_of * jnp.repeat(jnp.exp(steps), dims[dim] // shards_of).reshape((-1,) + (1,) * (len(dims) - 1 - dim))
    return factor_of


def gaussian(key, extent, spread, most, shards=(), kind=jnp.bfloat16):
    level = levels(key, extent, shards, -0.22, 0.18) if shards else 1.0
    values = jax.random.normal(key, extent, jnp.float32) * spread * level
    return jnp.minimum(jnp.maximum(values, -most), most).astype(kind)


def noise_with(rng, extent, scale, limit, cuts, heavy, dtype=jnp.bfloat16):
    drawn = scale * jax.random.normal(rng, extent, jnp.float32)
    if cuts:
        drawn = drawn * levels(rng, extent, cuts, -0.22, 0.18)
    return jnp.clip(strengthened(drawn, jax.random.fold_in(rng, 3), *heavy), -limit, limit).astype(dtype)


def setup_inputs(seed: int = 0, part: int = 0) -> dict:
    streams_of = jax.random.split(jax.random.key(seed), 17)
    own_keys = jax.random.split(jax.random.fold_in(streams_of[16], part), 17)
    return {
        "tokens": draw_tokens(jax.random.fold_in(jax.random.fold_in(streams_of[16], part), 71), part),
        "memory": gaussian(own_keys[1], (BATCH, HEADS, HEAD_DIM * HEAD_DIM), 0.5, 3.0, ((0, 16),), jnp.float32),
        "mix_gain": jnp.clip(1.0 + 0.18 * jax.random.normal(streams_of[2], (D,), jnp.float32), 0.1, 1.9),
        "w_query": gaussian(streams_of[3], (D, HEADS * HEAD_DIM), D ** -0.5, 0.125, ((1, 8),)),
        "w_key": gaussian(streams_of[4], (D, HEADS * HEAD_DIM), D ** -0.5, 0.125, ((1, 8),)),
        "w_value": gaussian(streams_of[5], (D, HEADS * HEAD_DIM), D ** -0.5, 0.125, ((1, 8),)),
        "w_gate": gaussian(streams_of[6], (D, HEADS * HEAD_DIM), D ** -0.5, 0.125, ((1, 8),)),
        "w_beta": gaussian(streams_of[7], (D, HEADS), D ** -0.5, 0.125),
        "w_decay": gaussian(streams_of[8], (D, HEADS), D ** -0.5, 0.125),
        "decay_rate": jnp.clip(jnp.exp(jax.random.uniform(streams_of[9], (HEADS,), jnp.float32, math.log(0.1), math.log(3.0))), 0.1, 3.0),
        "decay_bias": jnp.clip(jax.random.uniform(streams_of[10], (HEADS,), jnp.float32, -2.0, 1.0), -2.0, 1.0),
        "head_gain": jnp.clip(1.0 + 0.18 * jax.random.normal(streams_of[11], (HEAD_DIM,), jnp.float32), 0.1, 1.9),
        "w_out": gaussian(streams_of[12], (HEADS * HEAD_DIM, D), (HEADS * HEAD_DIM) ** -0.5, 0.15625, ((1, 8),)),
        "ffn_gain": jnp.clip(1.0 + 0.18 * jax.random.normal(streams_of[13], (D,), jnp.float32), 0.1, 1.9),
        "w_up": gaussian(streams_of[14], (D, FF), D ** -0.5, 0.125, ((1, 8),)),
        "w_down": noise_with(streams_of[15], (FF, D), FF ** -0.5, 0.09375, ((0, 8),), (0, 1, 8, 2.0)),
    }


epsilon = 1e-06

def delta_step(queries, keys_in, values, gates, strength, log_decay, memory, head_gain):
    count = queries.shape[0]
    heads = strength.shape[1]
    size = head_gain.shape[0]
    highest = lax.Precision.HIGHEST
    query_wide = queries.astype(jnp.float32).reshape(count, heads, size)
    key_wide = keys_in.astype(jnp.float32).reshape(count, heads, size)
    value_wide = values.astype(jnp.float32).reshape(count, heads, size)
    gate_wide = gates.astype(jnp.float32).reshape(count, heads, size)
    unit_key = key_wide * lax.rsqrt(lax.optimization_barrier(jnp.sum(key_wide * key_wide, axis=-1, keepdims=True)) + epsilon)
    matrix = memory.reshape(count, heads, size, size)
    recall = jnp.einsum('bhk,bhkv->bhv', unit_key, matrix, precision=highest)
    retain = jnp.exp(log_decay)[:, :, None, None]
    scaled = strength[:, :, None]
    erased = matrix - jnp.einsum('bhk,bhv->bhkv', unit_key, scaled * recall, precision=highest)
    written = jnp.einsum('bhk,bhv->bhkv', unit_key, scaled * value_wide, precision=highest)
    updated = retain * erased + written
    readout = jnp.einsum('bhk,bhkv->bhv', query_wide, updated, precision=highest)
    normed = readout * lax.rsqrt(lax.optimization_barrier(jnp.mean(readout * readout, axis=-1, keepdims=True)) + epsilon)
    normed = normed * head_gain * jax.nn.silu(gate_wide)
    return (updated.reshape(count, heads, size * size), normed.reshape(count, heads * size).astype(jnp.bfloat16))

def reference(tokens, memory, mix_gain, w_query, w_key, w_value, w_gate, w_beta, w_decay, decay_rate, decay_bias, head_gain, w_out, ffn_gain, w_up, w_down):
    width = tokens.shape[1]
    wide = tokens.astype(jnp.float32)
    scale_in = lax.rsqrt(lax.optimization_barrier(jnp.sum(wide * wide, axis=1)) / width + epsilon)[:, None]
    lifted_in = (wide * mix_gain).astype(jnp.bfloat16)

    def project(weight):
        return jnp.dot(lifted_in, weight, preferred_element_type=jnp.float32) * scale_in
    queries = project(w_query).astype(jnp.bfloat16)
    keys_in = project(w_key).astype(jnp.bfloat16)
    values = project(w_value).astype(jnp.bfloat16)
    gates = project(w_gate).astype(jnp.bfloat16)
    strength = jax.nn.sigmoid(project(w_beta))
    log_decay = -decay_rate * jax.nn.softplus(project(w_decay) + decay_bias)
    updated, mixed = delta_step(queries, keys_in, values, gates, strength, log_decay, memory, head_gain)
    branch = jnp.dot(mixed, w_out, preferred_element_type=jnp.float32)
    middle = (wide + branch).astype(jnp.bfloat16)
    middle_wide = middle.astype(jnp.float32)
    scale_mid = lax.rsqrt(lax.optimization_barrier(jnp.sum(middle_wide * middle_wide, axis=1)) / width + epsilon)[:, None]
    lifted_mid = (middle_wide * ffn_gain).astype(jnp.bfloat16)
    hidden = jnp.square(jax.nn.relu(jnp.dot(lifted_mid, w_up, preferred_element_type=jnp.float32) * scale_mid))
    hidden = hidden.astype(jnp.bfloat16)
    layer_out = (middle_wide + jnp.dot(hidden, w_down, preferred_element_type=jnp.float32)).astype(jnp.bfloat16)
    return (layer_out, updated)
```

```python
import functools

import jax
import jax.numpy as jnp
from jax import lax
from jax.experimental import pallas as pl
from jax.experimental.pallas import tpu as pltpu
from jax.sharding import PartitionSpec as P

epsilon = 1e-06
MESH = pl.DeviceIdType.MESH
f32 = jnp.float32
bf16 = jnp.bfloat16


def dot(a, b):
    return jnp.dot(a, b, preferred_element_type=f32)


def column(row):
    h = row.shape[1]
    wide = jnp.broadcast_to(row, (h, h))
    same = lax.broadcasted_iota(jnp.int32, (h, h), 0) == lax.broadcasted_iota(jnp.int32, (h, h), 1)
    return jnp.sum(jnp.where(same, wide, 0.0), axis=1, keepdims=True)


def offsets_of(kvs, tps):
    order = [0]
    for step in range(1, kvs):
        for a in (step, kvs - step):
            if a not in order:
                order.append(a)
    return [(a, b) for a in order for b in range(tps) if (a, b) != (0, 0)]


def kernel(
    kvs,
    tps,
    tokens,
    memory,
    mix_gain,
    w_query,
    w_key,
    w_value,
    w_gate,
    w_beta,
    w_decay,
    decay_rate,
    decay_bias,
    head_gain,
    w_out,
    ffn_gain,
    w_up,
    w_down,
    out,
    new_memory,
    tok_v,
    mem_v,
    mix_v,
    wq_v,
    wk_v,
    wv_v,
    wg_v,
    wb_v,
    wd_v,
    rate_v,
    bias_v,
    hgain_v,
    wout_v,
    fgain_v,
    wup_v,
    wdown_v,
    land_a,
    send_b,
    land_b,
    send_c,
    land_c,
    send_d,
    land_d,
    send_e,
    land_e,
    local_sem,
    send_sem,
    recv_sem,
):
    n = kvs * tps
    rows, w = tok_v.shape
    owned, heads, _ = mem_v.shape
    size = hgain_v.shape[1]
    width = n * w
    kv = lax.axis_index("kv")
    tp = lax.axis_index("tp")
    me = kv * tps + tp
    offsets = offsets_of(kvs, tps)

    def target(offset):
        return {"kv": lax.rem(kv + offset[0], kvs), "tp": lax.rem(tp + offset[1], tps)}

    def lane_of(where):
        return where["kv"] * tps + where["tp"]

    def source(offset):
        return lane_of(
            {"kv": lax.rem(kv + kvs - offset[0], kvs), "tp": lax.rem(tp + tps - offset[1], tps)}
        )

    hbm = (tokens, w_query, w_key, w_value, w_gate, w_beta, w_decay, mix_gain)
    hbm += (decay_rate, decay_bias, head_gain, memory, w_out, ffn_gain, w_up, w_down)
    vmem = (tok_v, wq_v, wk_v, wv_v, wg_v, wb_v, wd_v, mix_v)
    vmem += (rate_v, bias_v, hgain_v, mem_v, wout_v, fgain_v, wup_v, wdown_v)
    loads = [pltpu.make_async_copy(a, b, local_sem.at[i]) for i, (a, b) in enumerate(zip(hbm, vmem))]
    for load in loads:
        load.start()

    barrier = pltpu.get_barrier_semaphore()
    for offset in offsets:
        pl.semaphore_signal(barrier, inc=1, device_id=target(offset), device_id_type=MESH)
    pl.semaphore_wait(barrier, n - 1)

    def exchange(phase, outgoing, landing):
        copies = []
        for i, offset in reversed(list(enumerate(offsets))):
            where = target(offset)
            copy = pltpu.make_async_remote_copy(
                src_ref=outgoing(lane_of(where)),
                dst_ref=landing.at[me],
                send_sem=send_sem.at[phase, i],
                recv_sem=recv_sem.at[phase, i],
                device_id=where,
                device_id_type=MESH,
            )
            copy.start()
            copies.append(copy)
        return copies[::-1]

    loads[0].wait()
    copies_a = exchange(0, lambda lane: tok_v, land_a)
    for load in loads[1:8]:
        load.wait()
    mats = (wq_v, wk_v, wv_v, wg_v, wb_v, wd_v)

    def lift(piece, gain_v, lane):
        wide = piece.astype(f32)
        return (wide * gain_v[lane]).astype(bf16), jnp.sum(wide * wide, axis=1, keepdims=True)

    def project(piece, gain_v, lane, weights):
        lifted, squares = lift(piece, gain_v, lane)
        start = pl.multiple_of(lane * w, w)
        return [dot(lifted, weight[pl.ds(start, w), :]) for weight in weights] + [squares]

    totals = project(tok_v[...], mix_v, me, mats)
    for copy, offset in zip(copies_a, offsets):
        copy.wait_recv()
        src = source(offset)
        terms = project(land_a[src], mix_v, src, mats)
        totals = [a + b for a, b in zip(totals, terms)]
    scale_in = lax.rsqrt(totals[6] / width + epsilon)
    q, k, v, g, beta, decay = [total * scale_in for total in totals[:6]]
    for lane in range(n):
        for o in range(owned):
            r = lane * owned + o
            stacked = jnp.concatenate([x[r : r + 1] for x in (q, k, v, g)], axis=0)
            send_b[lane, o] = stacked.astype(bf16)
    copies_b = exchange(1, lambda lane: send_b.at[lane], land_b)
    land_b[me] = send_b[me]

    for load in loads[8:12]:
        load.wait()
    rate = column(rate_v[...])
    bias = column(bias_v[...])
    row_at = lax.broadcasted_iota(jnp.int32, (rows, heads), 0)
    strengths, retains = [], []
    for o in range(owned):
        mine = row_at == me * owned + o
        own_beta = column(jnp.sum(jnp.where(mine, beta, 0.0), axis=0, keepdims=True))
        own_decay = column(jnp.sum(jnp.where(mine, decay, 0.0), axis=0, keepdims=True))
        strengths.append(jax.nn.sigmoid(own_beta))
        x = own_decay + bias
        softplus = jnp.maximum(x, 0.0) + jnp.log1p(jnp.exp(-jnp.abs(x)))
        retains.append(jnp.exp(-rate * softplus))

    for copy in copies_b:
        copy.wait_recv()
    writes = []
    for o in range(owned):
        flat = jnp.concatenate([land_b[lane, o].astype(f32) for lane in range(n)], axis=1)
        query, key, value, gate = [
            jnp.concatenate([flat[i : i + 1, h * size : (h + 1) * size] for h in range(heads)], axis=0)
            for i in range(4)
        ]
        unit = key * lax.rsqrt(jnp.sum(key * key, axis=1, keepdims=True) + epsilon)
        recalls = [jnp.zeros((heads, size), f32) for _ in range(2)]
        reads = [jnp.zeros((heads, size), f32) for _ in range(2)]
        for i in range(size):
            row = mem_v[o, :, i * size : (i + 1) * size]
            recalls[i % 2] += unit[:, i : i + 1] * row
            reads[i % 2] += query[:, i : i + 1] * row
        recall = recalls[0] + recalls[1]
        read = reads[0] + reads[1]
        update = strengths[o] * (value - retains[o] * recall)
        readout = retains[o] * read + jnp.sum(query * unit, axis=1, keepdims=True) * update
        normed = readout * lax.rsqrt(jnp.mean(readout * readout, axis=1, keepdims=True) + epsilon)
        normed = normed * hgain_v[...] * (gate * jax.nn.sigmoid(gate))
        send_c[o] = normed.astype(bf16)
        writes.append((unit, update))
    copies_c = exchange(2, lambda lane: send_c, land_c)
    land_c[me] = send_c[...]

    for o in range(owned):
        unit, update = writes[o]
        for i in range(size):
            part = slice(i * size, (i + 1) * size)
            new_memory[o, :, part] = retains[o] * mem_v[o, :, part] + unit[:, i : i + 1] * update

    loads[12].wait()
    for copy in copies_c:
        copy.wait_recv()
    blocks = [land_c[lane, o].astype(f32) for lane in range(n) for o in range(owned)]
    mixed = jnp.concatenate(
        [jnp.concatenate([block[h : h + 1] for block in blocks], axis=0) for h in range(heads)], axis=1
    ).astype(bf16)
    branch = dot(mixed, wout_v[...])
    middle = (tok_v[...].astype(f32) + branch).astype(bf16)
    send_d[...] = middle
    copies_d = exchange(3, lambda lane: send_d, land_d)

    for load in loads[13:15]:
        load.wait()
    totals = project(middle, fgain_v, me, (wup_v,))
    for copy, offset in zip(copies_d, offsets):
        copy.wait_recv()
        src = source(offset)
        terms = project(land_d[src], fgain_v, src, (wup_v,))
        totals = [a + b for a, b in zip(totals, terms)]
    scale_mid = lax.rsqrt(totals[1] / width + epsilon)
    hidden = jnp.square(jnp.maximum(totals[0] * scale_mid, 0.0)).astype(bf16)

    loads[15].wait()
    chunk = w if w % 128 == 0 else width
    for first in range(0, width, chunk):
        terms = dot(hidden, wdown_v[:, first : first + chunk]).astype(bf16)
        for c in range(0, chunk, w):
            send_e[(first + c) // w] = terms[:, c : c + w]
    copies_e = exchange(4, lambda lane: send_e.at[lane], land_e)
    down = send_e[me].astype(f32)
    for copy, offset in zip(copies_e, offsets):
        copy.wait_recv()
        down = down + land_e[source(offset)].astype(f32)
    out[...] = (middle.astype(f32) + down).astype(bf16)
    for copies in (copies_a, copies_b, copies_c, copies_d, copies_e):
        for copy in copies:
            copy.wait_send()


def per_device(kvs, tps, *args):
    (tokens, memory, mix_gain, w_query, w_key, w_value, w_gate, w_beta, w_decay) = args[:9]
    (decay_rate, decay_bias, head_gain, w_out, ffn_gain, w_up, w_down) = args[9:]
    n = kvs * tps
    rows, w = tokens.shape
    owned, heads, _ = memory.shape
    size = head_gain.shape[0]
    columns = w_query.shape[1]
    operands = (
        tokens,
        memory,
        mix_gain.reshape(n, 1, w),
        w_query,
        w_key,
        w_value,
        w_gate,
        w_beta,
        w_decay,
        decay_rate.reshape(1, heads),
        decay_bias.reshape(1, heads),
        head_gain.reshape(1, size),
        w_out,
        ffn_gain.reshape(n, 1, w),
        w_up,
        w_down,
    )
    scratch = [pltpu.VMEM(x.shape, x.dtype) for x in operands]
    scratch += [
        pltpu.VMEM((n, rows, w), bf16),
        pltpu.VMEM((n, owned, 4, columns), bf16),
        pltpu.VMEM((n, owned, 4, columns), bf16),
        pltpu.VMEM((owned, heads, size), bf16),
        pltpu.VMEM((n, owned, heads, size), bf16),
        pltpu.VMEM((rows, w), bf16),
        pltpu.VMEM((n, rows, w), bf16),
        pltpu.VMEM((n, rows, w), bf16),
        pltpu.VMEM((n, rows, w), bf16),
        pltpu.SemaphoreType.DMA((len(operands),)),
        pltpu.SemaphoreType.DMA((5, n - 1)),
        pltpu.SemaphoreType.DMA((5, n - 1)),
    ]
    return pl.pallas_call(
        functools.partial(kernel, kvs, tps),
        out_shape=(
            jax.ShapeDtypeStruct((rows, w), bf16),
            jax.ShapeDtypeStruct(memory.shape, f32),
        ),
        in_specs=[pl.BlockSpec(memory_space=pltpu.HBM)] * len(operands),
        out_specs=(
            pl.BlockSpec(memory_space=pltpu.VMEM),
            pl.BlockSpec(memory_space=pltpu.VMEM),
        ),
        scratch_shapes=scratch,
        compiler_params=pltpu.CompilerParams(
            collective_id=0, has_side_effects=True, vmem_limit_bytes=48 * 1024 * 1024
        ),
    )(*operands)


def solution(mesh):
    placed = (
        P(("grp", "dp"), ("kv", "tp")),
        P(("grp", "dp", "kv", "tp"), None, None),
        P(),
        P(None, ("kv", "tp")),
        P(None, ("kv", "tp")),
        P(None, ("kv", "tp")),
        P(None, ("kv", "tp")),
        P(),
        P(),
        P(),
        P(),
        P(),
        P(None, ("kv", "tp")),
        P(),
        P(None, ("kv", "tp")),
        P(("kv", "tp"), None),
    )
    return jax.shard_map(
        functools.partial(per_device, mesh.shape["kv"], mesh.shape["tp"]),
        mesh=mesh,
        in_specs=placed,
        out_specs=(P(("grp", "dp"), ("kv", "tp")), P(("grp", "dp", "kv", "tp"), None, None)),
        check_vma=False,
    )
```

```python
import functools

import jax
import jax.numpy as jnp
from jax import lax
from jax.experimental import pallas as pl
from jax.experimental.pallas import tpu as pltpu
from jax.sharding import PartitionSpec as P

epsilon = 1e-06
MESH = pl.DeviceIdType.MESH
f32 = jnp.float32
bf16 = jnp.bfloat16


def dot(a, b):
    return jnp.dot(a, b, preferred_element_type=f32)


def dot_across(a, b):
    return lax.dot_general(a, b, (((1,), (1,)), ((), ())), preferred_element_type=f32)


def column(row):
    h = row.shape[1]
    wide = jnp.broadcast_to(row, (h, h))
    same = lax.broadcasted_iota(jnp.int32, (h, h), 0) == lax.broadcasted_iota(jnp.int32, (h, h), 1)
    return jnp.sum(jnp.where(same, wide, 0.0), axis=1, keepdims=True)


def offsets_of(kvs, tps):
    order = [0]
    for step in range(1, kvs):
        for a in (step, kvs - step):
            if a not in order:
                order.append(a)
    return [(a, b) for a in order for b in range(tps) if (a, b) != (0, 0)]


def kernel(
    kvs,
    tps,
    tokens,
    memory,
    mix_gain,
    w_query,
    w_key,
    w_value,
    w_gate,
    w_beta,
    w_decay,
    decay_rate,
    decay_bias,
    head_gain,
    w_out,
    ffn_gain,
    w_up,
    w_down,
    out,
    new_memory,
    tok_v,
    mem_v,
    mix_v,
    wq_v,
    wk_v,
    wv_v,
    wg_v,
    wb_v,
    wd_v,
    rate_v,
    bias_v,
    hgain_v,
    wout_v,
    fgain_v,
    wup_v,
    wdown_v,
    land_a,
    send_b,
    land_b,
    send_c,
    land_c,
    send_d,
    land_d,
    send_e,
    land_e,
    local_sem,
    send_sem,
    recv_sem,
):
    n = kvs * tps
    rows, w = tok_v.shape
    owned, heads, size, _ = mem_v.shape
    width = n * w
    kv = lax.axis_index("kv")
    tp = lax.axis_index("tp")
    me = kv * tps + tp
    offsets = offsets_of(kvs, tps)

    def target(offset):
        return {"kv": lax.rem(kv + offset[0], kvs), "tp": lax.rem(tp + offset[1], tps)}

    def lane_of(where):
        return where["kv"] * tps + where["tp"]

    def source(offset):
        return lane_of(
            {"kv": lax.rem(kv + kvs - offset[0], kvs), "tp": lax.rem(tp + tps - offset[1], tps)}
        )

    hbm = (tokens, w_query, w_key, w_value, w_gate, w_beta, w_decay, mix_gain)
    hbm += (decay_rate, decay_bias, head_gain, memory, w_out, ffn_gain, w_up, w_down)
    vmem = (tok_v, wq_v, wk_v, wv_v, wg_v, wb_v, wd_v, mix_v)
    vmem += (rate_v, bias_v, hgain_v, mem_v, wout_v, fgain_v, wup_v, wdown_v)
    loads = [pltpu.make_async_copy(a, b, local_sem.at[i]) for i, (a, b) in enumerate(zip(hbm, vmem))]
    for load in loads:
        load.start()

    barrier = pltpu.get_barrier_semaphore()
    for offset in offsets:
        pl.semaphore_signal(barrier, inc=1, device_id=target(offset), device_id_type=MESH)
    pl.semaphore_wait(barrier, n - 1)

    def exchange(phase, outgoing, landing):
        copies = []
        for i, offset in reversed(list(enumerate(offsets))):
            where = target(offset)
            copy = pltpu.make_async_remote_copy(
                src_ref=outgoing(lane_of(where)),
                dst_ref=landing.at[me],
                send_sem=send_sem.at[phase, i],
                recv_sem=recv_sem.at[phase, i],
                device_id=where,
                device_id_type=MESH,
            )
            copy.start()
            copies.append(copy)
        return copies[::-1]

    loads[0].wait()
    copies_a = exchange(0, lambda lane: tok_v, land_a)
    for load in loads[1:8]:
        load.wait()
    mats = (wq_v, wk_v, wv_v, wg_v, wb_v, wd_v)

    def lift(piece, gain_v, lane):
        wide = piece.astype(f32)
        return (wide * gain_v[lane]).astype(bf16), jnp.sum(wide * wide, axis=1, keepdims=True)

    def project(piece, gain_v, lane, weights, across):
        lifted, squares = lift(piece, gain_v, lane)
        part = pl.ds(pl.multiple_of(lane * w, w), w)
        if across:
            return [dot_across(lifted, weight[:, part]) for weight in weights] + [squares]
        return [dot(lifted, weight[part, :]) for weight in weights] + [squares]

    def project_all(own, landing, copies, gain_v, weights, across):
        if w % 128 == 0:
            totals = project(own, gain_v, me, weights, across)
            for copy, offset in zip(copies, offsets):
                copy.wait_recv()
                src = source(offset)
                terms = project(landing[src], gain_v, src, weights, across)
                totals = [a + b for a, b in zip(totals, terms)]
            return totals
        landing[me] = own
        for copy in copies:
            copy.wait_recv()
        lifts = [lift(landing[lane], gain_v, lane) for lane in range(n)]
        lifted = jnp.concatenate([a.astype(f32) for a, _ in lifts], axis=1).astype(bf16)
        squares = sum(b for _, b in lifts)
        return [(dot_across if across else dot)(lifted, weight[...]) for weight in weights] + [squares]

    totals = project_all(tok_v[...], land_a, copies_a, mix_v, mats, True)
    scale_in = lax.rsqrt(totals[6] / width + epsilon)
    q, k, v, g, beta, decay = [total * scale_in for total in totals[:6]]
    for lane in range(n):
        for o in range(owned):
            r = lane * owned + o
            stacked = jnp.concatenate([x[r : r + 1] for x in (q, k, v, g)], axis=0)
            send_b[lane, o] = stacked.astype(bf16)
    copies_b = exchange(1, lambda lane: send_b.at[lane], land_b)
    land_b[me] = send_b[me]

    for load in loads[8:12]:
        load.wait()
    rate = column(rate_v[...])
    bias = column(bias_v[...])
    row_at = lax.broadcasted_iota(jnp.int32, (rows, heads), 0)
    strengths, retains = [], []
    for o in range(owned):
        mine = row_at == me * owned + o
        own_beta = column(jnp.sum(jnp.where(mine, beta, 0.0), axis=0, keepdims=True))
        own_decay = column(jnp.sum(jnp.where(mine, decay, 0.0), axis=0, keepdims=True))
        strengths.append(jax.nn.sigmoid(own_beta))
        x = own_decay + bias
        softplus = jnp.maximum(x, 0.0) + jnp.log1p(jnp.exp(-jnp.abs(x)))
        retains.append(jnp.exp(-rate * softplus))

    for copy in copies_b:
        copy.wait_recv()
    writes = []
    for o in range(owned):
        flat = jnp.concatenate([land_b[lane, o].astype(f32) for lane in range(n)], axis=1)
        query, key, value, gate = [
            jnp.concatenate([flat[i : i + 1, h * size : (h + 1) * size] for h in range(heads)], axis=0)
            for i in range(4)
        ]
        unit = key * lax.rsqrt(jnp.sum(key * key, axis=1, keepdims=True) + epsilon)
        unit_t, query_t = unit.T, query.T
        recalls, reads = [], []
        for h in range(heads):
            matrix = mem_v[o, h]
            recalls.append(jnp.sum(unit_t[:, h : h + 1] * matrix, axis=0, keepdims=True))
            reads.append(jnp.sum(query_t[:, h : h + 1] * matrix, axis=0, keepdims=True))
        recall = jnp.concatenate(recalls, axis=0)
        read = jnp.concatenate(reads, axis=0)
        update = strengths[o] * (value - retains[o] * recall)
        readout = retains[o] * read + jnp.sum(query * unit, axis=1, keepdims=True) * update
        normed = readout * lax.rsqrt(jnp.mean(readout * readout, axis=1, keepdims=True) + epsilon)
        normed = normed * hgain_v[...] * (gate * jax.nn.sigmoid(gate))
        send_c[o] = normed.astype(bf16)
        writes.append((unit_t, update))
    copies_c = exchange(2, lambda lane: send_c, land_c)
    land_c[me] = send_c[...]

    for o in range(owned):
        unit_t, update = writes[o]
        for h in range(heads):
            kept = retains[o][h : h + 1] * mem_v[o, h]
            mem_v[o, h] = kept + unit_t[:, h : h + 1] * update[h : h + 1]
    store = pltpu.make_async_copy(mem_v, new_memory, local_sem.at[len(loads)])
    store.start()

    loads[12].wait()
    for copy in copies_c:
        copy.wait_recv()
    blocks = [land_c[lane, o].astype(f32) for lane in range(n) for o in range(owned)]
    mixed = jnp.concatenate(
        [jnp.concatenate([block[h : h + 1] for block in blocks], axis=0) for h in range(heads)], axis=1
    ).astype(bf16)
    branch = dot(mixed, wout_v[...])
    middle = (tok_v[...].astype(f32) + branch).astype(bf16)
    send_d[...] = middle
    copies_d = exchange(3, lambda lane: send_d, land_d)

    for load in loads[13:15]:
        load.wait()
    totals = project_all(middle, land_d, copies_d, fgain_v, (wup_v,), False)
    scale_mid = lax.rsqrt(totals[1] / width + epsilon)
    hidden = jnp.square(jnp.maximum(totals[0] * scale_mid, 0.0)).astype(bf16)

    loads[15].wait()
    chunk = w if w % 128 == 0 else width
    for first in range(0, width, chunk):
        terms = dot(hidden, wdown_v[:, first : first + chunk]).astype(bf16)
        for c in range(0, chunk, w):
            send_e[(first + c) // w] = terms[:, c : c + w]
    copies_e = exchange(4, lambda lane: send_e.at[lane], land_e)
    down = send_e[me].astype(f32)
    for copy, offset in zip(copies_e, offsets):
        copy.wait_recv()
        down = down + land_e[source(offset)].astype(f32)
    out[...] = (middle.astype(f32) + down).astype(bf16)
    store.wait()
    for copies in (copies_a, copies_b, copies_c, copies_d, copies_e):
        for copy in copies:
            copy.wait_send()


def per_device(kvs, tps, *args):
    (tokens, memory, mix_gain, w_query, w_key, w_value, w_gate, w_beta, w_decay) = args[:9]
    (decay_rate, decay_bias, head_gain, w_out, ffn_gain, w_up, w_down) = args[9:]
    n = kvs * tps
    rows, w = tokens.shape
    owned, heads, _ = memory.shape
    size = head_gain.shape[0]
    columns = w_query.shape[1]
    operands = (
        tokens,
        memory.reshape(owned, heads, size, size),
        mix_gain.reshape(n, 1, w),
        w_query.T,
        w_key.T,
        w_value.T,
        w_gate.T,
        w_beta.T,
        w_decay.T,
        decay_rate.reshape(1, heads),
        decay_bias.reshape(1, heads),
        head_gain.reshape(1, size),
        w_out,
        ffn_gain.reshape(n, 1, w),
        w_up,
        w_down,
    )
    scratch = [pltpu.VMEM(x.shape, x.dtype) for x in operands]
    scratch += [
        pltpu.VMEM((n, rows, w), bf16),
        pltpu.VMEM((n, owned, 4, columns), bf16),
        pltpu.VMEM((n, owned, 4, columns), bf16),
        pltpu.VMEM((owned, heads, size), bf16),
        pltpu.VMEM((n, owned, heads, size), bf16),
        pltpu.VMEM((rows, w), bf16),
        pltpu.VMEM((n, rows, w), bf16),
        pltpu.VMEM((n, rows, w), bf16),
        pltpu.VMEM((n, rows, w), bf16),
        pltpu.SemaphoreType.DMA((len(operands) + 1,)),
        pltpu.SemaphoreType.DMA((5, n - 1)),
        pltpu.SemaphoreType.DMA((5, n - 1)),
    ]
    layer_out, updated = pl.pallas_call(
        functools.partial(kernel, kvs, tps),
        out_shape=(
            jax.ShapeDtypeStruct((rows, w), bf16),
            jax.ShapeDtypeStruct((owned, heads, size, size), f32),
        ),
        in_specs=[pl.BlockSpec(memory_space=pltpu.HBM)] * len(operands),
        out_specs=(
            pl.BlockSpec(memory_space=pltpu.VMEM),
            pl.BlockSpec(memory_space=pltpu.HBM),
        ),
        scratch_shapes=scratch,
        compiler_params=pltpu.CompilerParams(
            collective_id=0, has_side_effects=True, vmem_limit_bytes=65 * 1000 * 1000
        ),
    )(*operands)
    return layer_out, updated.reshape(memory.shape)


def solution(mesh):
    placed = (
        P(("grp", "dp"), ("kv", "tp")),
        P(("grp", "dp", "kv", "tp"), None, None),
        P(),
        P(None, ("kv", "tp")),
        P(None, ("kv", "tp")),
        P(None, ("kv", "tp")),
        P(None, ("kv", "tp")),
        P(),
        P(),
        P(),
        P(),
        P(),
        P(None, ("kv", "tp")),
        P(),
        P(None, ("kv", "tp")),
        P(("kv", "tp"), None),
    )
    return jax.shard_map(
        functools.partial(per_device, mesh.shape["kv"], mesh.shape["tp"]),
        mesh=mesh,
        in_specs=placed,
        out_specs=(P(("grp", "dp"), ("kv", "tp")), P(("grp", "dp", "kv", "tp"), None, None)),
        check_vma=False,
    )
```

```python
import functools

import jax
import jax.numpy as jnp
from jax import lax
from jax.experimental import pallas as pl
from jax.experimental.pallas import tpu as pltpu
from jax.sharding import PartitionSpec as P

epsilon = 1e-06
MESH = pl.DeviceIdType.MESH
f32 = jnp.float32
bf16 = jnp.bfloat16


def dot(a, b):
    return jnp.dot(a, b, preferred_element_type=f32)


def dot_across(a, b):
    return lax.dot_general(a, b, (((1,), (1,)), ((), ())), preferred_element_type=f32)


def column(row):
    h = row.shape[1]
    wide = jnp.broadcast_to(row, (h, h))
    same = lax.broadcasted_iota(jnp.int32, (h, h), 0) == lax.broadcasted_iota(jnp.int32, (h, h), 1)
    return jnp.sum(jnp.where(same, wide, 0.0), axis=1, keepdims=True)


def offsets_of(kvs, tps):
    order = [0]
    for step in range(1, kvs):
        for a in (step, kvs - step):
            if a not in order:
                order.append(a)
    return [(a, b) for a in order for b in range(tps) if (a, b) != (0, 0)]


def kernel(
    kvs,
    tps,
    tokens,
    memory,
    mix_gain,
    w_query,
    w_key,
    w_value,
    w_gate,
    w_beta,
    w_decay,
    decay_rate,
    decay_bias,
    head_gain,
    w_out,
    ffn_gain,
    w_up,
    w_down,
    out,
    new_memory,
    tok_v,
    mem_v,
    mix_v,
    wq_v,
    wk_v,
    wv_v,
    wg_v,
    wb_v,
    wd_v,
    rate_v,
    bias_v,
    hgain_v,
    wout_v,
    fgain_v,
    wup_v,
    wdown_v,
    land_a,
    send_b,
    land_b,
    send_c,
    land_c,
    send_d,
    land_d,
    send_e,
    land_e,
    local_sem,
    send_sem,
    recv_sem,
):
    n = kvs * tps
    rows, w = tok_v.shape
    owned, heads, size, _ = mem_v.shape
    width = n * w
    kv = lax.axis_index("kv")
    tp = lax.axis_index("tp")
    me = kv * tps + tp
    offsets = offsets_of(kvs, tps)

    def target(offset):
        return {"kv": lax.rem(kv + offset[0], kvs), "tp": lax.rem(tp + offset[1], tps)}

    def lane_of(where):
        return where["kv"] * tps + where["tp"]

    def source(offset):
        return lane_of(
            {"kv": lax.rem(kv + kvs - offset[0], kvs), "tp": lax.rem(tp + tps - offset[1], tps)}
        )

    hbm = (tokens, w_query, w_key, w_value, w_gate, w_beta, w_decay, mix_gain)
    hbm += (decay_rate, decay_bias, head_gain, memory, w_out, ffn_gain, w_up, w_down)
    vmem = (tok_v, wq_v, wk_v, wv_v, wg_v, wb_v, wd_v, mix_v)
    vmem += (rate_v, bias_v, hgain_v, mem_v, wout_v, fgain_v, wup_v, wdown_v)
    loads = [pltpu.make_async_copy(a, b, local_sem.at[i]) for i, (a, b) in enumerate(zip(hbm, vmem))]
    for load in loads[:8]:
        load.start()

    barrier = pltpu.get_barrier_semaphore()
    for offset in offsets:
        pl.semaphore_signal(barrier, inc=1, device_id=target(offset), device_id_type=MESH)
    pl.semaphore_wait(barrier, n - 1)

    def exchange(phase, outgoing, landing):
        copies = []
        for i, offset in reversed(list(enumerate(offsets))):
            where = target(offset)
            copy = pltpu.make_async_remote_copy(
                src_ref=outgoing(lane_of(where)),
                dst_ref=landing.at[me],
                send_sem=send_sem.at[phase, i],
                recv_sem=recv_sem.at[phase, i],
                device_id=where,
                device_id_type=MESH,
            )
            copy.start()
            copies.append(copy)
        return copies[::-1]

    loads[0].wait()
    copies_a = exchange(0, lambda lane: tok_v, land_a)
    for load in loads[8:]:
        load.start()
    for load in loads[1:8]:
        load.wait()
    mats = (wq_v, wk_v, wv_v, wg_v, wb_v, wd_v)

    def lift(piece, gain_v, lane):
        wide = piece.astype(f32)
        return wide * gain_v[lane], jnp.sum(wide * wide, axis=1, keepdims=True)

    def project_all(own, landing, copies, gain_v, weights, across):
        landing[me] = own
        for copy in copies:
            copy.wait_recv()
        lifts = [lift(landing[lane], gain_v, lane) for lane in range(n)]
        lifted = jnp.concatenate([a for a, _ in lifts], axis=1).astype(bf16)
        squares = sum(b for _, b in lifts)
        return [(dot_across if across else dot)(lifted, weight[...]) for weight in weights] + [squares]

    totals = project_all(tok_v[...], land_a, copies_a, mix_v, mats, True)
    scale_in = lax.rsqrt(totals[6] / width + epsilon)
    q, k, v, g, beta, decay = [total * scale_in for total in totals[:6]]
    for lane in range(n):
        for o in range(owned):
            r = lane * owned + o
            stacked = jnp.concatenate([x[r : r + 1] for x in (q, k, v, g)], axis=0)
            send_b[lane, o] = stacked.astype(bf16)
    copies_b = exchange(1, lambda lane: send_b.at[lane], land_b)
    land_b[me] = send_b[me]

    for load in loads[8:12]:
        load.wait()
    rate = column(rate_v[...])
    bias = column(bias_v[...])
    row_at = lax.broadcasted_iota(jnp.int32, (rows, heads), 0)
    strengths, retains = [], []
    for o in range(owned):
        mine = row_at == me * owned + o
        own_beta = column(jnp.sum(jnp.where(mine, beta, 0.0), axis=0, keepdims=True))
        own_decay = column(jnp.sum(jnp.where(mine, decay, 0.0), axis=0, keepdims=True))
        strengths.append(jax.nn.sigmoid(own_beta))
        x = own_decay + bias
        softplus = jnp.maximum(x, 0.0) + jnp.log1p(jnp.exp(-jnp.abs(x)))
        retains.append(jnp.exp(-rate * softplus))

    for copy in copies_b:
        copy.wait_recv()
    writes = []
    for o in range(owned):
        flat = jnp.concatenate([land_b[lane, o].astype(f32) for lane in range(n)], axis=1)
        query, key, value, gate = [
            jnp.concatenate([flat[i : i + 1, h * size : (h + 1) * size] for h in range(heads)], axis=0)
            for i in range(4)
        ]
        unit = key * lax.rsqrt(jnp.sum(key * key, axis=1, keepdims=True) + epsilon)
        unit_t, query_t = unit.T, query.T
        recalls, reads = [], []
        for h in range(heads):
            matrix = mem_v[o, h]
            recalls.append(jnp.sum(unit_t[:, h : h + 1] * matrix, axis=0, keepdims=True))
            reads.append(jnp.sum(query_t[:, h : h + 1] * matrix, axis=0, keepdims=True))
        recall = jnp.concatenate(recalls, axis=0)
        read = jnp.concatenate(reads, axis=0)
        update = strengths[o] * (value - retains[o] * recall)
        readout = retains[o] * read + jnp.sum(query * unit, axis=1, keepdims=True) * update
        normed = readout * lax.rsqrt(jnp.mean(readout * readout, axis=1, keepdims=True) + epsilon)
        normed = normed * hgain_v[...] * (gate * jax.nn.sigmoid(gate))
        send_c[o] = normed.astype(bf16)
        writes.append((unit_t, update))
    copies_c = exchange(2, lambda lane: send_c, land_c)
    land_c[me] = send_c[...]

    for o in range(owned):
        unit_t, update = writes[o]
        for h in range(heads):
            kept = retains[o][h : h + 1] * mem_v[o, h]
            mem_v[o, h] = kept + unit_t[:, h : h + 1] * update[h : h + 1]
    store = pltpu.make_async_copy(mem_v, new_memory, local_sem.at[len(loads)])
    store.start()

    loads[12].wait()
    for copy in copies_c:
        copy.wait_recv()
    blocks = [land_c[lane, o].astype(f32) for lane in range(n) for o in range(owned)]
    mixed = jnp.concatenate(
        [jnp.concatenate([block[h : h + 1] for block in blocks], axis=0) for h in range(heads)], axis=1
    ).astype(bf16)
    branch = dot(mixed, wout_v[...])
    middle = (tok_v[...].astype(f32) + branch).astype(bf16)
    send_d[...] = middle
    copies_d = exchange(3, lambda lane: send_d, land_d)

    for load in loads[13:15]:
        load.wait()
    totals = project_all(middle, land_d, copies_d, fgain_v, (wup_v,), False)
    scale_mid = lax.rsqrt(totals[1] / width + epsilon)
    hidden = jnp.square(jnp.maximum(totals[0] * scale_mid, 0.0)).astype(bf16)

    loads[15].wait()
    chunk = w if w % 128 == 0 else width
    for first in range(0, width, chunk):
        terms = dot(hidden, wdown_v[:, first : first + chunk]).astype(bf16)
        for c in range(0, chunk, w):
            send_e[(first + c) // w] = terms[:, c : c + w]
    copies_e = exchange(4, lambda lane: send_e.at[lane], land_e)
    down = send_e[me].astype(f32)
    for copy, offset in zip(copies_e, offsets):
        copy.wait_recv()
        down = down + land_e[source(offset)].astype(f32)
    out[...] = (middle.astype(f32) + down).astype(bf16)
    store.wait()
    for copies in (copies_a, copies_b, copies_c, copies_d, copies_e):
        for copy in copies:
            copy.wait_send()


def finish(a, b, a_out, b_out, a_v, b_v, sem):
    owned, heads = b.shape[:2]
    parts = [(a, a_v, a_out)]
    for o in range(owned):
        for h in range(heads):
            parts.append((b.at[o, h], b_v.at[o, h], b_out.at[o, h]))
    into = [pltpu.make_async_copy(x, y, sem.at[0, i]) for i, (x, y, _) in enumerate(parts)]
    back = [pltpu.make_async_copy(y, z, sem.at[1, i]) for i, (_, y, z) in enumerate(parts)]
    for copy in into:
        copy.start()
    for first, second in zip(into, back):
        first.wait()
        second.start()
    for copy in back:
        copy.wait()


def per_device(kvs, tps, *args):
    (tokens, memory, mix_gain, w_query, w_key, w_value, w_gate, w_beta, w_decay) = args[:9]
    (decay_rate, decay_bias, head_gain, w_out, ffn_gain, w_up, w_down) = args[9:]
    n = kvs * tps
    rows, w = tokens.shape
    owned, heads, _ = memory.shape
    size = head_gain.shape[0]
    columns = w_query.shape[1]
    operands = (
        tokens,
        memory.reshape(owned, heads, size, size),
        mix_gain.reshape(n, 1, w),
        w_query.T,
        w_key.T,
        w_value.T,
        w_gate.T,
        w_beta.T,
        w_decay.T,
        decay_rate.reshape(1, heads),
        decay_bias.reshape(1, heads),
        head_gain.reshape(1, size),
        w_out,
        ffn_gain.reshape(n, 1, w),
        w_up,
        w_down,
    )
    scratch = [pltpu.VMEM(x.shape, x.dtype) for x in operands]
    scratch += [
        pltpu.VMEM((n, rows, w), bf16),
        pltpu.VMEM((n, owned, 4, columns), bf16),
        pltpu.VMEM((n, owned, 4, columns), bf16),
        pltpu.VMEM((owned, heads, size), bf16),
        pltpu.VMEM((n, owned, heads, size), bf16),
        pltpu.VMEM((rows, w), bf16),
        pltpu.VMEM((n, rows, w), bf16),
        pltpu.VMEM((n, rows, w), bf16),
        pltpu.VMEM((n, rows, w), bf16),
        pltpu.SemaphoreType.DMA((len(operands) + 1,)),
        pltpu.SemaphoreType.DMA((5, n - 1)),
        pltpu.SemaphoreType.DMA((5, n - 1)),
    ]
    layer_out, updated = pl.pallas_call(
        functools.partial(kernel, kvs, tps),
        out_shape=(
            jax.ShapeDtypeStruct((rows, w), bf16),
            jax.ShapeDtypeStruct((owned, heads, size, size), f32),
        ),
        in_specs=[pl.BlockSpec(memory_space=pltpu.HBM)] * len(operands),
        out_specs=(
            pl.BlockSpec(memory_space=pltpu.VMEM),
            pl.BlockSpec(memory_space=pltpu.HBM),
        ),
        scratch_shapes=scratch,
        compiler_params=pltpu.CompilerParams(
            collective_id=0, has_side_effects=True, vmem_limit_bytes=65 * 1000 * 1000
        ),
    )(*operands)
    layer_out, updated = pl.pallas_call(
        finish,
        out_shape=(
            jax.ShapeDtypeStruct(layer_out.shape, layer_out.dtype),
            jax.ShapeDtypeStruct(updated.shape, updated.dtype),
        ),
        in_specs=[pl.BlockSpec(memory_space=pltpu.HBM)] * 2,
        out_specs=(pl.BlockSpec(memory_space=pltpu.HBM),) * 2,
        scratch_shapes=[
            pltpu.VMEM(layer_out.shape, layer_out.dtype),
            pltpu.VMEM(updated.shape, updated.dtype),
            pltpu.SemaphoreType.DMA((2, 1 + owned * heads)),
        ],
        compiler_params=pltpu.CompilerParams(vmem_limit_bytes=65 * 1000 * 1000),
    )(layer_out, updated)
    return layer_out, updated.reshape(memory.shape)


def solution(mesh):
    placed = (
        P(("grp", "dp"), ("kv", "tp")),
        P(("grp", "dp", "kv", "tp"), None, None),
        P(),
        P(None, ("kv", "tp")),
        P(None, ("kv", "tp")),
        P(None, ("kv", "tp")),
        P(None, ("kv", "tp")),
        P(),
        P(),
        P(),
        P(),
        P(),
        P(None, ("kv", "tp")),
        P(),
        P(None, ("kv", "tp")),
        P(("kv", "tp"), None),
    )
    return jax.shard_map(
        functools.partial(per_device, mesh.shape["kv"], mesh.shape["tp"]),
        mesh=mesh,
        in_specs=placed,
        out_specs=(P(("grp", "dp"), ("kv", "tp")), P(("grp", "dp", "kv", "tp"), None, None)),
        check_vma=False,
    )
```
